32 devices in a mesh: ep: 8 (over z, x), tp: 4 (over y, core).
Axes of the slice: x: 2, y: 2, z: 4, core: 2. Of those that a mesh axis runs over, the one named last changes fastest.
Arguments:
- tokens: bfloat16 [1024, 2048], P('ep', 'tp'), may hold values from -36 to 36
- cotangent: bfloat16 [1024, 2048], P('ep', 'tp'), may hold values from -6 to 6
- routes: int32 [1024, 2], P('ep'), may hold values from 0 to 7, all different within a row; in each aligned block of 128 rows (0 to 127, 128 to 255, ...) at most 33 rows name the same one
- route_weights: bfloat16 [1024, 2], P('ep'), may hold values from 0.099609375 to 1
- gate_weight: bfloat16 [8, 2048, 1024], P('ep', None, 'tp'), may hold values from -0.125 to 0.125
- up_weight: bfloat16 [8, 2048, 1024], P('ep', None, 'tp'), may hold values from -0.125 to 0.125
- down_weight: bfloat16 [8, 1024, 2048], P('ep', 'tp'), may hold values from -0.1875 to 0.1875
Outputs:
- token_grad: bfloat16 [1024, 2048], P('ep', 'tp')
- weight_grad: bfloat16 [1024, 2], P('ep')
- down_grad: bfloat16 [8, 1024, 2048], P('ep', 'tp')
The draws below stay inside these ranges and needn't reach their ends.
Inputs may be any that keep to these rules, and one draw needn't show every extreme that they name: `routes`: each row names 2 different experts; within the rows of one device of ep (aligned blocks of 128 rows) no expert is named more than 33 times.
All inputs are finite; a program needn't handle non-finite values.
Results may differ from the reference program's by a relative error of at most 0.013.
Values may be sent and summed in bfloat16 or wider, within the bound.
A program may use at most 64 MiB of HBM per device.

```python
import math
import jax
import jax.numpy as jnp
import numpy as np
from jax import lax

D = 2048
F = 1024
TOPK = 2
TOK_DEV = 128
EXPERTS = 8
CAP = 33
TOKENS = 1024
N_EP = 8
N_TP = 4


def draw_tokens(key, part):
    values = jax.random.truncated_normal(key, -6.0, 6.0, (TOKENS, D), jnp.float32)
    return values.astype(jnp.bfloat16)


def block_scale(key, shape, split, least, high):
    factor_of, own = 1.0, jax.random.fold_in(key, 6)
    for position, shards_of in split:
        draws = jnp.exp(jax.random.uniform(jax.random.fold_in(own, position), (shards_of,), jnp.float32, least / len(split), high / len(split)))
        factor_of = factor_of * jnp.repeat(draws, shape[position] // shards_of).reshape([-1 if axis == position else 1 for axis in range(len(shape))])
    return factor_of


def routed_block(rng, own, number, rows, amount, top, bound, lean):
    ranking = jax.random.permutation(rng, amount)
    crowded, common = portions_of(amount, rows * top, bound, lean, True), portions_of(amount, rows * top, bound, lean, False)
    places = jnp.arange(amount)

    def named(sizes, offset_by):
        used = int((sizes > 0).sum())
        fixed = max(1, used // 4)
        moved = fixed + (places - fixed + offset_by * (used - fixed)) % max(1, amount - fixed)
        return jnp.zeros((amount,), jnp.int32).at[ranking[jnp.where(places < fixed, places, moved)]].set(jnp.asarray(sizes, jnp.int32))

    sizes = jnp.where(number % 4 == 0, named(crowded, number // 4), named(common, number - number // 4 - 1))
    mixed = jax.random.permutation(jax.random.fold_in(own, 3), amount)
    giver, receiver = mixed[0:amount // 2 * 2:2], mixed[1:amount // 2 * 2:2]
    margin = jnp.minimum(sizes[giver] - 1, bound - sizes[receiver]) // 2
    margin = jnp.where((giver == ranking[0]) | (receiver == ranking[0]) | (sizes[receiver] == 0), 0, jnp.maximum(margin, 0))
    moved = jax.random.randint(jax.random.fold_in(own, 4), (amount // 2,), 0, 1 << 20) % (margin + 1)
    sizes = sizes.at[giver].add(-moved).at[receiver].add(moved)
    labels = jnp.searchsorted(jnp.cumsum(sizes), jnp.arange(rows * top), side="right").astype(jnp.int32)
    grid = labels.reshape(top, rows).T
    grid = grid[jax.random.permutation(jax.random.fold_in(own, 1), rows)]
    offset_by = jax.random.randint(jax.random.fold_in(own, 2), (rows, 1), 0, top)
    return jnp.take_along_axis(grid, (jnp.arange(top)[None, :] + offset_by) % top, axis=1)


def portions_of(number_of, total, most, skew, full):
    weights = [(1 << 20) // math.isqrt(rank ** skew) + 1 for rank in range(1, number_of + 1)]
    largest = most if full else min(most, max(-(-total // number_of), total * weights[0] // sum(weights)))
    least = 1 if total - largest >= number_of - 1 else 0
    counts, rest = [largest] + [least] * (number_of - 1), total - largest - least * (number_of - 1)
    while rest > 0:
        movable = [i for i in range(1, number_of) if counts[i] < largest] or [i for i in range(1, number_of) if counts[i] < most]
        pool, budget = sum([weights[i] for i in movable]), rest
        for i in movable:
            extra = min(most - counts[i], max(1, budget * weights[i] // pool), rest)
            counts[i] = counts[i] + extra
            rest = rest - extra
    return np.array(counts)


def noise(rng, extent, scale, bound, pieces=(), kind=jnp.bfloat16):
    values = jax.random.normal(rng, extent, jnp.float32) * scale
    if len(pieces) > 0:
        values = block_scale(rng, extent, pieces, -0.22, 0.18) * values
    return jnp.clip(values, min=-bound, max=bound).astype(kind)


def setup_inputs(seed: int = 0) -> dict:
    seeds = jax.random.split(jax.random.key(seed), 8)
    tokens = draw_tokens(jax.random.fold_in(seeds[7], 71), 0)
    cotangent = noise(seeds[1], (TOKENS, D), 1.0, 6.0, ((0, 8), (1, 4)))
    routes_keys = jax.random.split(jax.random.fold_in(seeds[2], 1), TOKENS // TOK_DEV)
    routes_turns = jax.random.permutation(jax.random.fold_in(seeds[2], 3), TOKENS // TOK_DEV)
    routes = jax.vmap(lambda own, number: routed_block(jax.random.fold_in(seeds[2], 2), own, number, TOK_DEV, EXPERTS, TOPK, CAP, 2))(routes_keys, routes_turns).reshape((TOKENS, TOPK))
    route_weights = jnp.clip(0.099609375 + 0.9003906 * jax.random.uniform(seeds[3], (TOKENS, TOPK), jnp.float32) ** block_scale(seeds[3], (TOKENS, TOPK), ((0, 8),), -0.2, 0.2), 0.099609375, 1.0).astype(jnp.bfloat16)
    gate_weight = noise(seeds[4], (EXPERTS, D, F), D ** -0.5, 0.125, ((0, 8), (2, 4)))
    up_weight = noise(seeds[5], (EXPERTS, D, F), D ** -0.5, 0.125, ((0, 8), (2, 4)))
    down_weight = noise(seeds[6], (EXPERTS, F, D), F ** -0.5, 0.1875, ((0, 8), (1, 4)))
    return {"tokens": tokens, "cotangent": cotangent, "routes": routes, "route_weights": route_weights, "gate_weight": gate_weight, "up_weight": up_weight, "down_weight": down_weight}


clamp_limit = 7.0
alpha_gate = 1.702


def ranks_within(route_block, experts):
    flat_routes = route_block.reshape(-1)
    onehot = (flat_routes[:, None] == jnp.arange(experts, dtype=jnp.int32)[None, :]).astype(jnp.int32)
    before = jnp.cumsum(onehot, axis=0) - onehot
    return jnp.sum(before * onehot, axis=1).astype(jnp.int32)


def expert_terms(exp_rows, exp_grads, scales, gate_mat, up_mat, down_mat):
    gate_pre = jnp.dot(exp_rows, gate_mat, preferred_element_type=jnp.float32)
    up_pre = jnp.dot(exp_rows, up_mat, preferred_element_type=jnp.float32)
    gate_clip = jnp.minimum(gate_pre, clamp_limit)
    up_clip = jnp.clip(up_pre, -clamp_limit, clamp_limit)
    sigmoid_gate = jax.nn.sigmoid(alpha_gate * gate_clip)
    swish_gate = gate_clip * sigmoid_gate
    hidden = (up_clip + 1.0) * swish_gate
    back_proj = lax.dot_general(exp_grads, down_mat, (((1,), (1,)), ((), ())), preferred_element_type=jnp.float32)
    scores = jnp.sum(hidden * back_proj, axis=1)
    weight_col = scales.astype(jnp.float32)[:, None]
    scaled = back_proj * weight_col
    slope = sigmoid_gate + alpha_gate * swish_gate * (1.0 - sigmoid_gate)
    gate_grad = jnp.where(gate_pre < clamp_limit, scaled * (up_clip + 1.0) * slope, 0.0).astype(jnp.bfloat16)
    up_grad = jnp.where(jnp.abs(up_pre) < clamp_limit, scaled * swish_gate, 0.0).astype(jnp.bfloat16)
    weighted = (hidden * weight_col).astype(jnp.bfloat16)
    down_part = lax.dot_general(weighted, exp_grads, (((0,), (0,)), ((), ())), preferred_element_type=jnp.float32)
    token_part = lax.dot_general(gate_grad, gate_mat, (((1,), (1,)), ((), ())), preferred_element_type=jnp.float32)
    token_part = token_part + lax.dot_general(up_grad, up_mat, (((1,), (1,)), ((), ())), preferred_element_type=jnp.float32)
    return token_part, scores, down_part


def reference(tokens, cotangent, routes, route_weights, gate_weight, up_weight, down_weight):
    experts = gate_weight.shape[0]
    slot_count = N_EP * CAP
    blocks = routes.reshape(N_EP, TOK_DEV, TOPK)
    slot_ranks = jax.vmap(lambda block: ranks_within(block, experts))(blocks).reshape(-1)
    flat_routes = routes.reshape(-1)
    source = jnp.arange(TOKENS * TOPK, dtype=jnp.int32) // (TOK_DEV * TOPK)
    slot_place = (flat_routes * slot_count + source * CAP + slot_ranks).astype(jnp.int32)
    slot_owner = jnp.full((experts * slot_count,), -1, jnp.int32)
    slot_owner = slot_owner.at[slot_place].set(jnp.arange(TOKENS * TOPK, dtype=jnp.int32)).reshape(experts, slot_count)
    flat_weights = route_weights.reshape(-1)
    width_block = F // N_TP

    def one_expert(inputs):
        slot_table, gate_mat, up_mat, down_mat = inputs
        filled = slot_table >= 0
        pair_index = jnp.where(filled, slot_table, 0)
        token_index = pair_index // TOPK
        exp_rows = jnp.where(filled[:, None], tokens[token_index], 0).astype(jnp.bfloat16)
        exp_grads = jnp.where(filled[:, None], cotangent[token_index], 0).astype(jnp.bfloat16)
        scales = jnp.where(filled, flat_weights[pair_index], 0).astype(jnp.bfloat16)
        token_total = jnp.zeros((slot_count, D), jnp.float32)
        score_total = jnp.zeros((slot_count,), jnp.float32)
        down_parts = []
        for part_index in range(N_TP):
            low = part_index * width_block
            token_part, scores, down_part = expert_terms(
                exp_rows, exp_grads, scales, gate_mat[:, low:low + width_block],
                up_mat[:, low:low + width_block], down_mat[low:low + width_block, :])
            token_total = token_total + token_part.astype(jnp.bfloat16).astype(jnp.float32)
            score_total = score_total + scores
            down_parts.append(down_part)
        down_full = jnp.concatenate(down_parts, axis=0)
        return token_total.astype(jnp.bfloat16), score_total, down_full.astype(jnp.bfloat16)

    token_parts, score_parts, down_grad = lax.map(one_expert, (slot_owner, gate_weight, up_weight, down_weight))
    gathered = token_parts.reshape(experts * slot_count, D)[slot_place].reshape(TOKENS, TOPK, D)
    token_grad = jnp.sum(gathered.astype(jnp.float32), axis=1).astype(jnp.bfloat16)
    weight_grad = score_parts.reshape(-1)[slot_place].reshape(TOKENS, TOPK).astype(jnp.bfloat16)
    return token_grad, weight_grad, down_grad
```

```python
import functools

import jax
import jax.numpy as jnp
from jax import lax
from jax.experimental import pallas as pl
from jax.experimental.pallas import tpu as pltpu
from jax.sharding import PartitionSpec as P

clamp_limit = 7.0
alpha_gate = 1.702
GROUPS = 1


def ranks_within(route_block, experts):
    flat_routes = route_block.reshape(-1)
    onehot = (flat_routes[:, None] == jnp.arange(experts, dtype=jnp.int32)[None, :]).astype(
        jnp.int32
    )
    before = jnp.cumsum(onehot, axis=0) - onehot
    return jnp.sum(before * onehot, axis=1)


def expert_terms(exp_rows, exp_grads, scales, gate_mat, up_mat, down_mat):
    gate_pre = jnp.dot(exp_rows, gate_mat, preferred_element_type=jnp.float32)
    up_pre = jnp.dot(exp_rows, up_mat, preferred_element_type=jnp.float32)
    gate_clip = jnp.minimum(gate_pre, clamp_limit)
    up_clip = jnp.clip(up_pre, -clamp_limit, clamp_limit)
    sigmoid_gate = jax.nn.sigmoid(alpha_gate * gate_clip)
    swish_gate = gate_clip * sigmoid_gate
    hidden = (up_clip + 1.0) * swish_gate
    back_proj = lax.dot_general(
        exp_grads, down_mat, (((1,), (1,)), ((), ())), preferred_element_type=jnp.float32
    )
    scores = jnp.sum(hidden * back_proj, axis=1)
    weight_col = scales.astype(jnp.float32)[:, None]
    scaled = back_proj * weight_col
    slope = sigmoid_gate + alpha_gate * swish_gate * (1.0 - sigmoid_gate)
    gate_grad = jnp.where(gate_pre < clamp_limit, scaled * (up_clip + 1.0) * slope, 0.0).astype(
        jnp.bfloat16
    )
    up_grad = jnp.where(jnp.abs(up_pre) < clamp_limit, scaled * swish_gate, 0.0).astype(
        jnp.bfloat16
    )
    weighted = (hidden * weight_col).astype(jnp.bfloat16)
    down_part = lax.dot_general(
        weighted, exp_grads, (((0,), (0,)), ((), ())), preferred_element_type=jnp.float32
    )
    token_part = lax.dot_general(
        gate_grad, gate_mat, (((1,), (1,)), ((), ())), preferred_element_type=jnp.float32
    )
    token_part = token_part + lax.dot_general(
        up_grad, up_mat, (((1,), (1,)), ((), ())), preferred_element_type=jnp.float32
    )
    return (token_part, scores, down_part)


def native(tokens, cotangent, routes, route_weights, gate_weight, up_weight, down_weight):
    experts = lax.axis_size("ep")
    tok_rows, top_count = routes.shape
    slots_each = tok_rows * top_count // experts + 1
    slot_count = experts * slots_each
    slot_ranks = ranks_within(routes, experts)
    slot_place = routes.reshape(-1) * slots_each + slot_ranks
    slot_owner = jnp.full((slot_count,), -1, jnp.int32)
    slot_owner = slot_owner.at[slot_place].set(jnp.arange(tok_rows * top_count, dtype=jnp.int32))
    filled = slot_owner >= 0
    pair_index = jnp.where(filled, slot_owner, 0)
    token_index = pair_index // top_count
    send_scales = jnp.where(filled, route_weights.reshape(-1)[pair_index], 0)
    send_rows = jnp.where(filled[:, None], tokens[token_index], 0)
    send_grads = jnp.where(filled[:, None], cotangent[token_index], 0)
    part_rows, part_grads, scales = (
        lax.all_to_all(send_rows, "ep", split_axis=0, concat_axis=0, tiled=True),
        lax.all_to_all(send_grads, "ep", split_axis=0, concat_axis=0, tiled=True),
        lax.all_to_all(send_scales, "ep", split_axis=0, concat_axis=0, tiled=True),
    )
    exp_rows, exp_grads = (
        lax.all_gather(part_rows, "tp", axis=1, tiled=True),
        lax.all_gather(part_grads, "tp", axis=1, tiled=True),
    )
    token_part, scores, down_part = expert_terms(
        exp_rows, exp_grads, scales, gate_weight[0], up_weight[0], down_weight[0]
    )
    token_share = lax.psum_scatter(
        token_part.astype(jnp.bfloat16), "tp", scatter_dimension=1, tiled=True
    )
    score_total = lax.psum(scores, "tp")
    back_rows, back_scores = (
        lax.all_to_all(token_share, "ep", split_axis=0, concat_axis=0, tiled=True),
        lax.all_to_all(
            score_total.astype(jnp.bfloat16), "ep", split_axis=0, concat_axis=0, tiled=True
        ),
    )
    pair_rows = back_rows[slot_place].reshape(tok_rows, top_count, back_rows.shape[1])
    token_grad = jnp.sum(pair_rows.astype(jnp.float32), axis=1).astype(jnp.bfloat16)
    weight_grad = back_scores[slot_place].reshape(tok_rows, top_count)
    return (token_grad, weight_grad, down_part.astype(jnp.bfloat16)[None])


def xor_index(value, mask):
    bit = 1
    while bit <= mask:
        if mask & bit:
            value = value + bit - 2 * bit * ((value // bit) % 2)
        bit *= 2
    return value


def dot_nn(a, b):
    return lax.dot_general(a, b, (((1,), (0,)), ((), ())), preferred_element_type=jnp.float32)


def dot_nt(a, b):
    return lax.dot_general(a, b, (((1,), (1,)), ((), ())), preferred_element_type=jnp.float32)


def dot_tn(a, b):
    return lax.dot_general(a, b, (((0,), (0,)), ((), ())), preferred_element_type=jnp.float32)


def fused_kernel(
    peers, main, spare, spare_rows, groups,
    tokens_ref, cotangent_ref, routes_ref, scale_ref, gate_hbm, up_hbm, down_hbm,
    token_out, weight_out, down_out,
    gate_v, up_v, down_v, send_main, send_spare, rows_all, spare_all,
    part, core_part, y_send, y_part, ret_send, ret_recv, ret_spare_send, ret_spare_recv,
    score_own, score_core, score_sum, score_y, score_send, score_recv, weighted_v, down_stage,
    w_sem, down_sem,
    disp_s, disp_r, disp_es, disp_er, y_s, y_r, y_es, y_er,
    core_s, core_r, core_es, core_er,
    rs_s, rs_r, ry_s, ry_r, sc_s, sc_r, sy_s, sy_r,
    ret_s, ret_r, ret_es, ret_er, ret_ss, ret_sr,
):
    f32, bf16 = jnp.float32, jnp.bfloat16
    ep = lax.axis_index("ep")
    tp = lax.axis_index("tp")
    yy, cc = tp // 2, tp % 2
    core_dev = {"tp": yy * 2 + 1 - cc}
    y_dev = {"tp": (1 - yy) * 2 + cc}
    other_y = 1 - yy

    def ep_dev(m):
        return {"ep": xor_index(ep, m)}

    barrier = pltpu.get_barrier_semaphore()
    devices = [ep_dev(m) for m in range(1, peers)] + [core_dev, y_dev]
    for device in devices:
        pl.semaphore_signal(
            barrier, inc=1, device_id=device, device_id_type=pl.DeviceIdType.MESH
        )
    loads = [
        pltpu.make_async_copy(gate_hbm.at[0], gate_v, w_sem.at[0]),
        pltpu.make_async_copy(up_hbm.at[0], up_v, w_sem.at[1]),
        pltpu.make_async_copy(down_hbm.at[0], down_v, w_sem.at[2]),
    ]
    for load in loads:
        load.start()

    tok = tokens_ref.shape[0]
    width = tokens_ref.shape[1]
    slots = peers * main + spare_rows
    lanes = 128

    def lane_iota(shape, dim):
        return lax.broadcasted_iota(jnp.int32, shape, dim)

    m_row = lane_iota((1, lanes), 1)
    e_row = jnp.zeros((1, lanes), jnp.int32)
    bit = 1
    while bit < peers:
        mine = (ep // bit) % 2
        have = jnp.where((m_row & bit) != 0, 1, 0)
        e_row = e_row + bit * (have + mine - 2 * have * mine)
        bit *= 2
    e_row = jnp.where(m_row < peers, e_row, -1)
    first = (routes_ref[:, 0:1] == e_row).astype(f32)
    second = (routes_ref[:, 1:2] == e_row).astype(f32)
    named = first + second
    tri = (lane_iota((tok, tok), 0) >= lane_iota((tok, tok), 1)).astype(bf16)
    rank1 = named * dot_nn(tri, named.astype(bf16))
    scale = scale_ref[...].astype(f32)
    scale_m = first * scale[:, 0:1] + second * scale[:, 1:2]

    s_mat = lane_iota((lanes, slots), 1)
    m_mat = lane_iota((lanes, slots), 0)
    base = peers * main
    in_main = (s_mat < base) & (s_mat >= m_mat * main) & (s_mat < m_mat * main + main)
    j_mat = s_mat - base
    in_spare = (j_mat >= m_mat * spare) & (j_mat < m_mat * spare + spare) & (j_mat < peers * spare) & (j_mat >= 0)
    expand = (in_main | in_spare).astype(f32).astype(bf16)
    s_row = lane_iota((1, slots), 1)
    t_main = s_row + 1
    t_spare = s_row - base + 1 + main
    for m in range(1, peers):
        t_main = t_main - jnp.where(s_row >= m * main, main, 0)
        t_spare = t_spare - jnp.where(s_row - base >= m * spare, spare, 0)
    target = jnp.where(s_row < base, t_main, jnp.where(s_row < base + peers * spare, t_spare, -5))
    ranks_s = dot_nn(rank1.astype(bf16), expand)
    pick = (ranks_s == target.astype(f32)).astype(f32).astype(bf16)

    x_slots = dot_tn(pick, tokens_ref[...])
    g_slots = dot_tn(pick, cotangent_ref[...])
    x_main = x_slots[:base].astype(bf16).reshape(peers, main, width)
    g_main = g_slots[:base].astype(bf16).reshape(peers, main, width)
    send_main[0] = x_main
    send_main[1] = g_main
    rows_all[0, tp, 0] = x_main[0]
    rows_all[1, tp, 0] = g_main[0]
    lane1 = (lane_iota((tok, lanes), 1) + 1).astype(f32)
    spare_h = 2 * spare + 1
    row_id = lane_iota((spare_h, width), 0)
    for m in range(peers):
        w_row = jnp.sum(
            jnp.where(rank1[:, m : m + 1] == lane1, scale_m[:, m : m + 1], 0.0), axis=0, keepdims=True
        )
        wide = jnp.concatenate([w_row, jnp.zeros((1, width - lanes), f32)], axis=1)
        block = jnp.broadcast_to(wide, (spare_h, width))
        for x in range(spare):
            j = base + m * spare + x
            block = jnp.where(row_id == x, x_slots[j : j + 1], block)
            block = jnp.where(row_id == spare + x, g_slots[j : j + 1], block)
        block = block.astype(bf16)
        send_spare[m] = block
        if m == 0:
            spare_all[tp, 0] = block

    pl.semaphore_wait(barrier, len(devices))

    pending = []

    def remote(src, dst, s_sem, r_sem, device):
        copy = pltpu.make_async_remote_copy(
            src_ref=src, dst_ref=dst, send_sem=s_sem, recv_sem=r_sem,
            device_id=device, device_id_type=pl.DeviceIdType.MESH,
        )
        copy.start()
        pending.append(copy)
        return copy

    disp = {}

    def dispatch(m):
        disp[m] = (
            remote(send_spare.at[m], spare_all.at[tp, m], disp_es.at[m], disp_er.at[m], ep_dev(m)),
            remote(send_main.at[:, m], rows_all.at[:, tp, m], disp_s.at[m], disp_r.at[m], ep_dev(m)),
        )

    y_copy, core_a, core_b = {}, {}, {}

    def forward(m):
        if m > 0:
            for copy in disp[m]:
                copy.wait_recv()
        if m > 0:
            src, src_e = rows_all.at[:, tp, m], spare_all.at[tp, m]
        else:
            src, src_e = send_main.at[:, 0], send_spare.at[0]
        dst, dst_e = rows_all.at[:, tp, m], spare_all.at[tp, m]
        y_copy[m] = (
            remote(src_e, dst_e, y_es.at[m], y_er.at[m], y_dev),
            remote(src, dst, y_s.at[m], y_r.at[m], y_dev),
        )
        core_a[m] = (
            remote(src_e, dst_e, core_es.at[0, m], core_er.at[0, m], core_dev),
            remote(src, dst, core_s.at[0, m], core_r.at[0, m], core_dev),
        )

    y_tp = other_y * 2 + cc

    def relay(m):
        for copy in y_copy[m]:
            copy.wait_recv()
        core_b[m] = (
            remote(spare_all.at[y_tp, m], spare_all.at[y_tp, m], core_es.at[1, m], core_er.at[1, m], core_dev),
            remote(rows_all.at[:, y_tp, m], rows_all.at[:, y_tp, m], core_s.at[1, m], core_r.at[1, m], core_dev),
        )

    def settle(m):
        for copy in core_a[m] + core_b[m]:
            copy.wait_recv()

    tp_size = rows_all.shape[1]
    eye = (lane_iota((main, lanes), 0) == lane_iota((main, lanes), 1))
    spare_row = lane_iota((spare_rows, 1), 0)
    wide_row = lane_iota((spare_rows, width), 0)
    lane_row = lane_iota((1, lanes), 1)

    def spare_tile(which, t):
        tile = jnp.zeros((spare_rows, width), f32)
        for m in range(peers):
            block = spare_all[t, m].astype(f32)
            for x in range(spare):
                row = which * spare + x
                tile = jnp.where(wide_row == m * spare + x, block[row : row + 1], tile)
        return tile.astype(bf16)

    spans = [(g * peers // groups, (g + 1) * peers // groups) for g in range(groups)]

    def rows_of(which, t, lo, hi):
        block = rows_all[which, t, lo:hi].reshape((hi - lo) * main, width)
        if hi == peers:
            block = jnp.concatenate([block, spare_tile(which, t)], axis=0)
        return block

    rs_copy, ry_copy, small = {}, {}, {}

    def compute(g):
        lo, hi = spans[g]
        last = hi == peers
        gate_pre = up_pre = back = None
        for t in range(tp_size):
            x_t = rows_of(0, t, lo, hi)
            g_t = rows_of(1, t, lo, hi)
            terms = (
                dot_nn(x_t, gate_v[t * width : (t + 1) * width, :]),
                dot_nn(x_t, up_v[t * width : (t + 1) * width, :]),
                dot_nt(g_t, down_v[:, t * width : (t + 1) * width]),
            )
            if t == 0:
                gate_pre, up_pre, back = terms
            else:
                gate_pre, up_pre, back = gate_pre + terms[0], up_pre + terms[1], back + terms[2]
        cols = []
        spare_col = jnp.zeros((spare_rows, 1), f32)
        for m in range(peers):
            w_row = spare_all[0, m].astype(f32)[2 * spare : 2 * spare + 1, 0:lanes]
            if lo <= m < hi:
                cols.append(jnp.sum(jnp.where(eye, w_row, 0.0), axis=1, keepdims=True))
            if last:
                for x in range(spare):
                    spare_col = jnp.where(
                        spare_row == m * spare + x, w_row[:, main + x : main + x + 1], spare_col
                    )
        if last:
            cols.append(spare_col)
        weight_col = jnp.concatenate(cols, axis=0)
        gate_clip = jnp.minimum(gate_pre, clamp_limit)
        up_clip = jnp.clip(up_pre, -clamp_limit, clamp_limit)
        sigmoid_gate = jax.nn.sigmoid(alpha_gate * gate_clip)
        swish_gate = gate_clip * sigmoid_gate
        hidden = (up_clip + 1.0) * swish_gate
        scores = jnp.sum(hidden * back, axis=1, keepdims=True)
        scaled = back * weight_col
        slope = sigmoid_gate + alpha_gate * swish_gate * (1.0 - sigmoid_gate)
        gate_grad = jnp.where(gate_pre < clamp_limit, scaled * (up_clip + 1.0) * slope, 0.0).astype(bf16)
        up_grad = jnp.where(jnp.abs(up_pre) < clamp_limit, scaled * swish_gate, 0.0).astype(bf16)
        row_lo, row_n = lo * main, gate_pre.shape[0]
        weighted_v[row_lo : row_lo + row_n, :] = (hidden * weight_col).astype(bf16)
        for m in range(lo, hi):
            col = scores[(m - lo) * main : (m - lo + 1) * main]
            score_own[m] = jnp.sum(jnp.where(eye, col, 0.0), axis=0, keepdims=True)
        if last:
            for m in range(peers):
                row = score_own[m]
                for x in range(spare):
                    j = (hi - lo) * main + m * spare + x
                    row = jnp.where(lane_row == main + x, scores[j : j + 1], row)
                score_own[m] = row
            small[0] = remote(score_own, score_core, sc_s, sc_r, core_dev)
        for t in range(tp_size):
            term = dot_nt(gate_grad, gate_v[t * width : (t + 1) * width, :])
            term = term + dot_nt(up_grad, up_v[t * width : (t + 1) * width, :])
            part[t // 2, t % 2, row_lo : row_lo + row_n, :] = term.astype(bf16)
        rows = pl.ds(row_lo, row_n)
        rs_copy[g] = remote(
            part.at[:, 1 - cc, rows], core_part.at[:, rows], rs_s.at[g], rs_r.at[g], core_dev
        )

    def span_rows(g):
        lo, hi = spans[g]
        return lo * main, (hi - lo) * main + (spare_rows if hi == peers else 0)

    def reduce_core(g):
        row_lo, row_n = span_rows(g)
        rows = pl.ds(row_lo, row_n)
        rs_copy[g].wait_recv()
        y_send[rows, :] = (
            part[other_y, cc, rows, :].astype(f32) + core_part[other_y, rows, :].astype(f32)
        ).astype(bf16)
        ry_copy[g] = remote(y_send.at[rows], y_part.at[rows], ry_s.at[g], ry_r.at[g], y_dev)
        if spans[g][1] == peers:
            small[0].wait_recv()
            score_sum[...] = score_own[...] + score_core[...]
            small[1] = remote(score_sum, score_y, sy_s, sy_r, y_dev)

    returns = {}

    def reduce_y(g):
        lo, hi = spans[g]
        row_lo, row_n = span_rows(g)
        rows = pl.ds(row_lo, row_n)
        ry_copy[g].wait_recv()
        total = (
            part[yy, cc, rows, :].astype(f32)
            + core_part[yy, rows, :].astype(f32)
            + y_part[rows, :].astype(f32)
        )
        ret_send[lo:hi] = total[: (hi - lo) * main].astype(bf16).reshape(hi - lo, main, width)
        returns[g] = []
        for m in range(max(lo, 1), hi):
            returns[g].append(remote(ret_send.at[m], ret_recv.at[m], ret_s.at[m], ret_r.at[m], ep_dev(m)))
        if hi == peers:
            small[1].wait_recv()
            score_send[...] = score_sum[...] + score_y[...]
            for m in range(peers):
                for x in range(spare):
                    j = (hi - lo) * main + m * spare + x
                    ret_spare_send[m, x : x + 1] = total[j : j + 1]
            for m in range(1, peers):
                returns[g].append(
                    remote(ret_spare_send.at[m], ret_spare_recv.at[m], ret_es.at[m], ret_er.at[m], ep_dev(m))
                )
                returns[g].append(
                    remote(score_send.at[m], score_recv.at[m], ret_ss.at[m], ret_sr.at[m], ep_dev(m))
                )

    for m in range(1, peers):
        dispatch(m)
    done = 0
    for g, (lo, hi) in enumerate(spans):
        for m in range(lo, hi):
            forward(m)
            if m > lo:
                relay(m - 1)
        relay(hi - 1)
        if g == 0:
            for load in loads:
                load.wait()
        if g > 0:
            reduce_core(g - 1)
        for m in range(lo, hi):
            settle(m)
        compute(g)
        if g > 0:
            reduce_y(g - 1)
    reduce_core(groups - 1)
    stores = []
    half = tp_size // 2
    def down_piece(t):
        g_t = rows_of(1, t, 0, peers)
        down_stage[:, t * width : (t + 1) * width] = dot_tn(weighted_v[...], g_t).astype(bf16)

    for t in range(half):
        down_piece(t)
    reduce_y(groups - 1)
    for t in range(half, tp_size):
        down_piece(t)
    store = pltpu.make_async_copy(down_stage, down_out.at[0], down_sem)
    store.start()

    for g in range(groups):
        for copy in returns[g]:
            copy.wait_recv()
    back_rows = [ret_send[0]] + [ret_recv[m] for m in range(1, peers)]
    tile = jnp.zeros((spare_rows, width), f32)
    pair0 = jnp.zeros((tok, lanes), f32)
    pair1 = jnp.zeros((tok, lanes), f32)
    for m in range(peers):
        block = ret_spare_send[0] if m == 0 else ret_spare_recv[m]
        for x in range(spare):
            tile = jnp.where(wide_row == m * spare + x, block[x : x + 1], tile)
        row = score_send[0] if m == 0 else score_recv[m]
        found = jnp.where(rank1[:, m : m + 1] == lane1, row, 0.0)
        pair0 = pair0 + first[:, m : m + 1] * found
        pair1 = pair1 + second[:, m : m + 1] * found
    back_all = jnp.concatenate(back_rows + [tile.astype(bf16)], axis=0)
    token_out[...] = dot_nn(pick, back_all).astype(bf16)
    col0 = jnp.sum(pair0, axis=1, keepdims=True)
    col1 = jnp.sum(pair1, axis=1, keepdims=True)
    two = lane_iota((tok, 2), 1)
    weight_out[...] = jnp.where(two == 0, col0, col1).astype(bf16)
    for copy in pending:
        copy.wait_send()
    store.wait()


def fused(tokens, cotangent, routes, route_weights, gate_weight, up_weight, down_weight):
    peers = lax.axis_size("ep")
    tp_size = lax.axis_size("tp")
    tok, top_count = routes.shape
    width = tokens.shape[1]
    cap = tok * top_count // peers + 1
    main = cap // 16 * 16
    spare = cap - main
    spare_rows = -(-(peers * spare) // 16) * 16
    groups = GROUPS
    total = peers * main + spare_rows
    hid, full = down_weight.shape[1], down_weight.shape[2]
    bf16, f32 = jnp.bfloat16, jnp.float32
    vm = pltpu.VMEM
    dma = pltpu.SemaphoreType.DMA
    any_spec = pl.BlockSpec(memory_space=pl.ANY)
    v_spec = pl.BlockSpec(memory_space=pltpu.VMEM)
    spare_h = 2 * spare + 1
    return pl.pallas_call(
        functools.partial(fused_kernel, peers, main, spare, spare_rows, groups),
        out_shape=(
            jax.ShapeDtypeStruct((tok, width), bf16),
            jax.ShapeDtypeStruct((tok, top_count), bf16),
            jax.ShapeDtypeStruct((1, hid, full), bf16),
        ),
        in_specs=[v_spec] * 4 + [any_spec] * 3,
        out_specs=(v_spec, v_spec, any_spec),
        scratch_shapes=[
            vm((full, hid), bf16), vm((full, hid), bf16), vm((hid, full), bf16),
            vm((2, peers, main, width), bf16), vm((peers, spare_h, width), bf16),
            vm((2, tp_size, peers, main, width), bf16), vm((tp_size, peers, spare_h, width), bf16),
            vm((2, 2, total, width), bf16), vm((2, total, width), bf16),
            vm((total, width), bf16), vm((total, width), bf16),
            vm((peers, main, width), bf16), vm((peers, main, width), bf16),
            vm((peers, spare, width), f32), vm((peers, spare, width), f32),
            vm((peers, 1, 128), f32), vm((peers, 1, 128), f32), vm((peers, 1, 128), f32),
            vm((peers, 1, 128), f32), vm((peers, 1, 128), f32), vm((peers, 1, 128), f32),
            vm((total, hid), bf16), vm((hid, full), bf16),
            dma((3,)), dma,
        ]
        + [dma((peers,))] * 8
        + [dma((2, peers))] * 4
        + [dma((groups,))] * 4
        + [dma] * 4
        + [dma((peers,))] * 6,
        compiler_params=pltpu.CompilerParams(
            collective_id=0, has_side_effects=True
        ),
    )(tokens, cotangent, routes, route_weights, gate_weight, up_weight, down_weight)


def per_device(tokens, cotangent, routes, route_weights, gate_weight, up_weight, down_weight):
    args = (tokens, cotangent, routes, route_weights, gate_weight, up_weight, down_weight)
    cap = routes.shape[0] * routes.shape[1] // lax.axis_size("ep") + 1
    peers = lax.axis_size("ep")
    small = cap < 16 or cap % 16 == 0 or cap > 127 or peers & (peers - 1) != 0
    if small or lax.axis_size("tp") != 4 or routes.shape[1] != 2:
        return native(*args)
    return fused(*args)


def solution(mesh):
    placed = (
        P("ep", "tp"),
        P("ep", "tp"),
        P("ep", None),
        P("ep", None),
        P("ep", None, "tp"),
        P("ep", None, "tp"),
        P("ep", "tp", None),
    )
    return jax.shard_map(
        per_device,
        mesh=mesh,
        in_specs=placed,
        out_specs=(P("ep", "tp"), P("ep", None), P("ep", "tp", None)),
        check_vma=False,
    )
```

```python
import functools

import jax
import jax.numpy as jnp
from jax import lax
from jax.experimental import pallas as pl
from jax.experimental.pallas import tpu as pltpu
from jax.sharding import PartitionSpec as P

clamp_limit = 7.0
alpha_gate = 1.702
send_order = (1, 2, 3, 4, 5, 6, 7)
relay_lag = 4


def ranks_within(route_block, experts):
    flat_routes = route_block.reshape(-1)
    onehot = (flat_routes[:, None] == jnp.arange(experts, dtype=jnp.int32)[None, :]).astype(
        jnp.int32
    )
    before = jnp.cumsum(onehot, axis=0) - onehot
    return jnp.sum(before * onehot, axis=1)


def expert_terms(exp_rows, exp_grads, scales, gate_mat, up_mat, down_mat):
    gate_pre = jnp.dot(exp_rows, gate_mat, preferred_element_type=jnp.float32)
    up_pre = jnp.dot(exp_rows, up_mat, preferred_element_type=jnp.float32)
    gate_clip = jnp.minimum(gate_pre, clamp_limit)
    up_clip = jnp.clip(up_pre, -clamp_limit, clamp_limit)
    sigmoid_gate = jax.nn.sigmoid(alpha_gate * gate_clip)
    swish_gate = gate_clip * sigmoid_gate
    hidden = (up_clip + 1.0) * swish_gate
    back_proj = lax.dot_general(
        exp_grads, down_mat, (((1,), (1,)), ((), ())), preferred_element_type=jnp.float32
    )
    scores = jnp.sum(hidden * back_proj, axis=1)
    weight_col = scales.astype(jnp.float32)[:, None]
    scaled = back_proj * weight_col
    slope = sigmoid_gate + alpha_gate * swish_gate * (1.0 - sigmoid_gate)
    gate_grad = jnp.where(gate_pre < clamp_limit, scaled * (up_clip + 1.0) * slope, 0.0).astype(
        jnp.bfloat16
    )
    up_grad = jnp.where(jnp.abs(up_pre) < clamp_limit, scaled * swish_gate, 0.0).astype(
        jnp.bfloat16
    )
    weighted = (hidden * weight_col).astype(jnp.bfloat16)
    down_part = lax.dot_general(
        weighted, exp_grads, (((0,), (0,)), ((), ())), preferred_element_type=jnp.float32
    )
    token_part = lax.dot_general(
        gate_grad, gate_mat, (((1,), (1,)), ((), ())), preferred_element_type=jnp.float32
    )
    token_part = token_part + lax.dot_general(
        up_grad, up_mat, (((1,), (1,)), ((), ())), preferred_element_type=jnp.float32
    )
    return (token_part, scores, down_part)


def native(tokens, cotangent, routes, route_weights, gate_weight, up_weight, down_weight):
    experts = lax.axis_size("ep")
    tok_rows, top_count = routes.shape
    slots_each = tok_rows * top_count // experts + 1
    slot_count = experts * slots_each
    slot_ranks = ranks_within(routes, experts)
    slot_place = routes.reshape(-1) * slots_each + slot_ranks
    slot_owner = jnp.full((slot_count,), -1, jnp.int32)
    slot_owner = slot_owner.at[slot_place].set(jnp.arange(tok_rows * top_count, dtype=jnp.int32))
    filled = slot_owner >= 0
    pair_index = jnp.where(filled, slot_owner, 0)
    token_index = pair_index // top_count
    send_scales = jnp.where(filled, route_weights.reshape(-1)[pair_index], 0)
    send_rows = jnp.where(filled[:, None], tokens[token_index], 0)
    send_grads = jnp.where(filled[:, None], cotangent[token_index], 0)
    part_rows, part_grads, scales = (
        lax.all_to_all(send_rows, "ep", split_axis=0, concat_axis=0, tiled=True),
        lax.all_to_all(send_grads, "ep", split_axis=0, concat_axis=0, tiled=True),
        lax.all_to_all(send_scales, "ep", split_axis=0, concat_axis=0, tiled=True),
    )
    exp_rows, exp_grads = (
        lax.all_gather(part_rows, "tp", axis=1, tiled=True),
        lax.all_gather(part_grads, "tp", axis=1, tiled=True),
    )
    token_part, scores, down_part = expert_terms(
        exp_rows, exp_grads, scales, gate_weight[0], up_weight[0], down_weight[0]
    )
    token_share = lax.psum_scatter(
        token_part.astype(jnp.bfloat16), "tp", scatter_dimension=1, tiled=True
    )
    score_total = lax.psum(scores, "tp")
    back_rows, back_scores = (
        lax.all_to_all(token_share, "ep", split_axis=0, concat_axis=0, tiled=True),
        lax.all_to_all(
            score_total.astype(jnp.bfloat16), "ep", split_axis=0, concat_axis=0, tiled=True
        ),
    )
    pair_rows = back_rows[slot_place].reshape(tok_rows, top_count, back_rows.shape[1])
    token_grad = jnp.sum(pair_rows.astype(jnp.float32), axis=1).astype(jnp.bfloat16)
    weight_grad = back_scores[slot_place].reshape(tok_rows, top_count)
    return (token_grad, weight_grad, down_part.astype(jnp.bfloat16)[None])


def xor_index(value, mask):
    bit = 1
    while bit <= mask:
        if mask & bit:
            value = value + bit - 2 * bit * ((value // bit) % 2)
        bit *= 2
    return value


def dot_nn(a, b):
    return lax.dot_general(a, b, (((1,), (0,)), ((), ())), preferred_element_type=jnp.float32)


def dot_nt(a, b):
    return lax.dot_general(a, b, (((1,), (1,)), ((), ())), preferred_element_type=jnp.float32)


def dot_tn(a, b):
    return lax.dot_general(a, b, (((0,), (0,)), ((), ())), preferred_element_type=jnp.float32)


def fused_kernel(
    peers, main, spare, spare_rows, order, chunks,
    tokens_ref, cotangent_ref, routes_ref, scale_ref, gate_hbm, up_hbm, down_hbm,
    token_out, weight_out, down_out,
    gate_v, up_v, down_v, send_main, send_spare, rows_all, spare_all,
    part, core_part, y_send, y_part, ret_send, ret_recv, ret_spare_send, ret_spare_recv,
    score_own, score_core, score_sum, score_y, score_send, score_recv, weighted_v,
    w_sem, disp_s, disp_r, disp_es, disp_er, y_s, y_r, y_es, y_er,
    core_s, core_r, core_es, core_er,
    rs_s, rs_r, ry_s, ry_r, sc_s, sc_r, sy_s, sy_r,
    ret_s, ret_r, ret_es, ret_er, ret_ss, ret_sr,
):
    f32, bf16 = jnp.float32, jnp.bfloat16
    ep = lax.axis_index("ep")
    tp = lax.axis_index("tp")
    yy, cc = tp // 2, tp % 2
    other_y, other_c = 1 - yy, 1 - cc
    core_tp, y_tp, far_tp = yy * 2 + other_c, other_y * 2 + cc, other_y * 2 + other_c
    core_dev, y_dev = {"tp": core_tp}, {"tp": y_tp}

    def ep_dev(m):
        return {"ep": xor_index(ep, m)}

    barrier = pltpu.get_barrier_semaphore()
    devices = [ep_dev(m) for m in range(1, peers)] + [core_dev, y_dev]
    for device in devices:
        pl.semaphore_signal(
            barrier, inc=1, device_id=device, device_id_type=pl.DeviceIdType.MESH
        )
    loads = [
        pltpu.make_async_copy(gate_hbm.at[0], gate_v, w_sem.at[0]),
        pltpu.make_async_copy(up_hbm.at[0], up_v, w_sem.at[1]),
        pltpu.make_async_copy(down_hbm.at[0], down_v, w_sem.at[2]),
    ]
    for load in loads:
        load.start()

    tok, width = tokens_ref.shape
    base = peers * main
    slots = base + spare_rows
    padded = score_own.shape[1]
    group = 16

    def iota(shape, dim):
        return lax.broadcasted_iota(jnp.int32, shape, dim)

    m_col = iota((group, 1), 0)
    e_col = jnp.zeros((group, 1), jnp.int32)
    bit = 1
    while bit < peers:
        mine = (ep // bit) % 2
        have = jnp.where((m_col & bit) != 0, 1, 0)
        e_col = e_col + bit * (have + mine - 2 * have * mine)
        bit *= 2
    e_col = jnp.where(m_col < peers, e_col, -1)
    first = (routes_ref[0:1, :] == e_col).astype(f32)
    second = (routes_ref[1:2, :] == e_col).astype(f32)
    named = first + second
    tri = (iota((tok, tok), 0) <= iota((tok, tok), 1)).astype(f32).astype(bf16)
    rank1 = named * dot_nn(named.astype(bf16), tri)
    scale = scale_ref[...].astype(f32)
    scale_m = (first * scale[0:1, :] + second * scale[1:2, :]).astype(bf16)

    def in_block(place, m):
        in_main = (place >= m * main) & (place < m * main + main)
        low = base + m * spare
        return in_main | ((place >= low) & (place < low + spare))

    expand = in_block(iota((slots, group), 0), iota((slots, group), 1))
    expand = (expand & (iota((slots, group), 1) < peers)).astype(f32).astype(bf16)
    s_col = iota((slots, 1), 0)
    t_main = s_col + 1
    t_spare = s_col - base + 1 + main
    for m in range(1, peers):
        t_main = t_main - jnp.where(s_col >= m * main, main, 0)
        t_spare = t_spare - jnp.where(s_col - base >= m * spare, spare, 0)
    target = jnp.where(s_col < base, t_main, jnp.where(s_col < base + peers * spare, t_spare, -5))
    ranks_s = dot_nn(expand, rank1.astype(bf16))
    pick = (ranks_s == target.astype(f32)).astype(f32).astype(bf16)
    pick_pad = jnp.concatenate([pick, jnp.zeros((padded - slots, tok), bf16)], axis=0)

    x_slots = dot_nn(pick, tokens_ref[...])
    x_main = x_slots[:base].astype(bf16).reshape(peers, main, width)
    send_main[0] = x_main
    rows_all[0, tp, 0] = x_main[0]
    g_slots = dot_nn(pick, cotangent_ref[...])
    g_main = g_slots[:base].astype(bf16).reshape(peers, main, width)
    send_main[1] = g_main
    rows_all[1, tp, 0] = g_main[0]
    w_rows = dot_nt(scale_m, pick_pad)
    w_rows = jnp.concatenate([w_rows, jnp.zeros((group, width - padded), f32)], axis=1)
    spare_h = 2 * spare + 1
    row_id = iota((spare_h, width), 0)
    for m in range(peers):
        block = jnp.broadcast_to(w_rows[m : m + 1], (spare_h, width))
        for x in range(spare):
            j = base + m * spare + x
            block = jnp.where(row_id == x, x_slots[j : j + 1], block)
            block = jnp.where(row_id == spare + x, g_slots[j : j + 1], block)
        block = block.astype(bf16)
        send_spare[m] = block
        if m == 0:
            spare_all[tp, 0] = block

    pl.semaphore_wait(barrier, len(devices))

    pending = []

    def remote(src, dst, s_sem, r_sem, device):
        copy = pltpu.make_async_remote_copy(
            src_ref=src, dst_ref=dst, send_sem=s_sem, recv_sem=r_sem,
            device_id=device, device_id_type=pl.DeviceIdType.MESH,
        )
        copy.start()
        pending.append(copy)
        return copy

    disp, y_copy, core_a, core_b = {}, {}, {}, {}

    def dispatch(w, m):
        disp[w, m] = [
            remote(send_main.at[w, m], rows_all.at[w, tp, m], disp_s.at[w, m], disp_r.at[w, m], ep_dev(m))
        ]
        if w == 0:
            disp[w, m].append(
                remote(send_spare.at[m], spare_all.at[tp, m], disp_es.at[m], disp_er.at[m], ep_dev(m))
            )

    def forward(w, m):
        if m > 0:
            for copy in disp[w, m]:
                copy.wait_recv()
        src = rows_all.at[w, tp, m] if m > 0 else send_main.at[w, 0]
        dst = rows_all.at[w, tp, m]
        y_copy[w, m] = [remote(src, dst, y_s.at[w, m], y_r.at[w, m], y_dev)]
        core_a[w, m] = [remote(src, dst, core_s.at[0, w, m], core_r.at[0, w, m], core_dev)]
        if w == 0:
            src = spare_all.at[tp, m] if m > 0 else send_spare.at[0]
            dst = spare_all.at[tp, m]
            y_copy[w, m].append(remote(src, dst, y_es.at[m], y_er.at[m], y_dev))
            core_a[w, m].append(remote(src, dst, core_es.at[0, m], core_er.at[0, m], core_dev))

    def relay(w, m):
        for copy in y_copy[w, m]:
            copy.wait_recv()
        block = rows_all.at[w, y_tp, m]
        core_b[w, m] = [remote(block, block, core_s.at[1, w, m], core_r.at[1, w, m], core_dev)]
        if w == 0:
            block = spare_all.at[y_tp, m]
            core_b[w, m].append(remote(block, block, core_es.at[1, m], core_er.at[1, m], core_dev))

    def settle(copies, w):
        for m in range(peers):
            for copy in copies[w, m]:
                copy.wait_recv()

    tp_size = rows_all.shape[1]
    wide_row = iota((spare_rows, width), 0)

    def spare_tile(which, t):
        tile = jnp.zeros((spare_rows, width), f32)
        for m in range(peers):
            block = spare_all[t, m].astype(f32)
            for x in range(spare):
                row = which * spare + x
                tile = jnp.where(wide_row == m * spare + x, block[row : row + 1], tile)
        return tile.astype(bf16)

    def rows_of(which, t):
        block = rows_all[which, t].reshape(base, width)
        return jnp.concatenate([block, spare_tile(which, t)], axis=0)

    def cut(t):
        return pl.ds(pl.multiple_of(t * width, width), width)

    for m in order:
        dispatch(0, m)
    for m in order:
        dispatch(1, m)
    turn = (0,) + order
    items = [(w, m) for w in range(2) for m in turn]
    sums = {}

    def add(name, term):
        sums[name] = sums[name] + term if name in sums else term

    def front(t):
        x_t = rows_of(0, t)
        add("gate", dot_nn(x_t, gate_v[cut(t), :]))
        add("up", dot_nn(x_t, up_v[cut(t), :]))

    def gates():
        gate_pre, up_pre = sums["gate"], sums["up"]
        s_lane = iota((1, padded), 1)
        w_row = jnp.zeros((1, padded), f32)
        for m in range(peers):
            row = spare_all[0, m].astype(f32)[2 * spare : 2 * spare + 1, 0:padded]
            w_row = jnp.where(in_block(s_lane, m), row, w_row)
        eye_b = (iota((slots, padded), 0) == iota((slots, padded), 1)).astype(f32).astype(bf16)
        weight_col = dot_nt(eye_b, jnp.broadcast_to(w_row, (group, padded)).astype(bf16))[:, 0:1]
        gate_clip = jnp.minimum(gate_pre, clamp_limit)
        up_clip = jnp.clip(up_pre, -clamp_limit, clamp_limit)
        sigmoid_gate = jax.nn.sigmoid(alpha_gate * gate_clip)
        swish_gate = gate_clip * sigmoid_gate
        hidden = (up_clip + 1.0) * swish_gate
        slope = sigmoid_gate + alpha_gate * swish_gate * (1.0 - sigmoid_gate)
        weighted_v[...] = (hidden * weight_col).astype(bf16)
        gate_fac = jnp.where(gate_pre < clamp_limit, weight_col * (up_clip + 1.0) * slope, 0.0)
        up_fac = jnp.where(jnp.abs(up_pre) < clamp_limit, weight_col * swish_gate, 0.0)
        return hidden, gate_fac, up_fac

    hooks = [
        (peers, lambda: front(tp)),
        (peers + 1, lambda: (settle(core_a, 0), front(core_tp))),
        (peers + relay_lag, lambda: front(y_tp)),
        (peers + relay_lag + 1, lambda: (settle(core_b, 0), front(far_tp))),
        (peers + relay_lag + 2, lambda: factors.append(gates())),
    ]
    factors = []
    for i in range(2 * peers + relay_lag):
        if i < 2 * peers:
            forward(*items[i])
        if i >= relay_lag:
            relay(*items[i - relay_lag])
        if i == peers:
            for load in loads:
                load.wait()
        for when, hook in hooks:
            if when == i:
                hook()
    hidden, gate_fac, up_fac = factors[0]
    back = dot_nt(rows_of(1, tp), down_v[:, cut(tp)])
    settle(core_a, 1)
    back = back + dot_nt(rows_of(1, core_tp), down_v[:, cut(core_tp)])
    back = back + dot_nt(rows_of(1, y_tp), down_v[:, cut(y_tp)])
    settle(core_b, 1)
    back = back + dot_nt(rows_of(1, far_tp), down_v[:, cut(far_tp)])
    gate_grad = (back * gate_fac).astype(bf16)
    up_grad = (back * up_fac).astype(bf16)

    def piece(t):
        return dot_nt(gate_grad, gate_v[cut(t), :]) + dot_nt(up_grad, up_v[cut(t), :])

    part[2] = piece(far_tp).astype(bf16)
    rs_far = remote(part.at[2], core_part.at[0], rs_s.at[0], rs_r.at[0], core_dev)
    part[3] = piece(core_tp).astype(bf16)
    rs_near = remote(part.at[3], core_part.at[1], rs_s.at[1], rs_r.at[1], core_dev)
    mine = piece(y_tp).astype(bf16).astype(f32)
    rs_far.wait_recv()
    y_send[...] = (mine + core_part[0].astype(f32)).astype(bf16)
    ry = []
    for q, (lo, hi) in enumerate(chunks):
        rows = pl.ds(lo * main, (hi - lo) * main + (spare_rows if hi == peers else 0))
        ry.append(remote(y_send.at[rows], y_part.at[rows], ry_s.at[q], ry_r.at[q], y_dev))
    scores = jnp.sum(hidden * back, axis=1, keepdims=True)
    eye = iota((slots, padded), 0) == iota((slots, padded), 1)
    score_own[...] = jnp.sum(jnp.where(eye, scores, 0.0), axis=0, keepdims=True)
    small = remote(score_own, score_core, sc_s, sc_r, core_dev)
    mine = piece(tp).astype(bf16).astype(f32)
    rs_near.wait_recv()
    part[0] = mine.astype(bf16)
    small.wait_recv()
    score_sum[...] = score_own[...] + score_core[...]
    small_y = remote(score_sum, score_y, sy_s, sy_r, y_dev)
    returns = []
    for q, (lo, hi) in enumerate(chunks):
        row_lo, row_n = lo * main, (hi - lo) * main
        row_n = row_n + (spare_rows if hi == peers else 0)
        ry[q].wait_recv()
        total = (
            part[0, row_lo : row_lo + row_n, :].astype(f32)
            + core_part[1, row_lo : row_lo + row_n, :].astype(f32)
            + y_part[row_lo : row_lo + row_n, :].astype(f32)
        )
        ret_send[lo:hi] = total[: (hi - lo) * main].astype(bf16).reshape(hi - lo, main, width)
        for m in range(max(lo, 1), hi):
            returns.append(remote(ret_send.at[m], ret_recv.at[m], ret_s.at[m], ret_r.at[m], ep_dev(m)))
        if hi == peers:
            for m in range(peers):
                for x in range(spare):
                    j = (hi - lo) * main + m * spare + x
                    ret_spare_send[m, x : x + 1] = total[j : j + 1]
            for m in range(1, peers):
                returns.append(
                    remote(ret_spare_send.at[m], ret_spare_recv.at[m], ret_es.at[m], ret_er.at[m], ep_dev(m))
                )
    small_y.wait_recv()
    score_send[...] = score_sum[...] + score_y[...]
    for m in range(1, peers):
        returns.append(remote(score_send, score_recv.at[m], ret_ss.at[m], ret_sr.at[m], ep_dev(m)))
    weighted = weighted_v[...]
    for t in range(tp_size):
        down_out[0, :, t * width : (t + 1) * width] = dot_tn(weighted, rows_of(1, t)).astype(bf16)
    for copy in returns:
        copy.wait_recv()
    back_rows = [ret_send[0]] + [ret_recv[m] for m in range(1, peers)]
    tile = jnp.zeros((spare_rows, width), f32)
    s_lane = iota((1, padded), 1)
    group_row = iota((group, padded), 0)
    score_mat = jnp.zeros((group, padded), f32)
    for m in range(peers):
        block = ret_spare_send[0] if m == 0 else ret_spare_recv[m]
        for x in range(spare):
            tile = jnp.where(wide_row == m * spare + x, block[x : x + 1], tile)
        row = score_send[...] if m == 0 else score_recv[m]
        score_mat = jnp.where(group_row == m, jnp.where(in_block(s_lane, m), row, 0.0), score_mat)
    back_all = jnp.concatenate(back_rows + [tile.astype(bf16)], axis=0)
    token_out[...] = dot_tn(pick, back_all).astype(bf16)
    found = dot_nn(score_mat.astype(bf16), pick_pad)
    row0 = jnp.sum(first * found, axis=0, keepdims=True)
    row1 = jnp.sum(second * found, axis=0, keepdims=True)
    weight_out[...] = jnp.where(iota((2, tok), 0) == 0, row0, row1).astype(bf16)
    for copy in pending:
        copy.wait_send()


def fused(tokens, cotangent, routes, route_weights, gate_weight, up_weight, down_weight):
    peers = lax.axis_size("ep")
    tp_size = lax.axis_size("tp")
    tok, top_count = routes.shape
    width = tokens.shape[1]
    cap = tok * top_count // peers + 1
    main = cap // 16 * 16
    spare = cap - main
    spare_rows = -(-(peers * spare) // 16) * 16
    total = peers * main + spare_rows
    padded = -(-total // 128) * 128
    hid, full = down_weight.shape[1], down_weight.shape[2]
    order = send_order if len(send_order) == peers - 1 else tuple(range(1, peers))
    pieces = min(4, peers)
    chunks = [(q * peers // pieces, (q + 1) * peers // pieces) for q in range(pieces)]
    bf16, f32 = jnp.bfloat16, jnp.float32
    vm = pltpu.VMEM
    dma = pltpu.SemaphoreType.DMA
    any_spec = pl.BlockSpec(memory_space=pl.ANY)
    v_spec = pl.BlockSpec(memory_space=pltpu.VMEM)
    spare_h = 2 * spare + 1
    token_grad, weight_grad, down_grad = pl.pallas_call(
        functools.partial(fused_kernel, peers, main, spare, spare_rows, order, chunks),
        out_shape=(
            pltpu.VMEM((tok, width), bf16),
            pltpu.VMEM((top_count, tok), bf16),
            pltpu.VMEM((1, hid, full), bf16),
        ),
        in_specs=[v_spec] * 4 + [any_spec] * 3,
        out_specs=(v_spec, v_spec, v_spec),
        scratch_shapes=[
            vm((full, hid), bf16), vm((full, hid), bf16), vm((hid, full), bf16),
            vm((2, peers, main, width), bf16), vm((peers, spare_h, width), bf16),
            vm((2, tp_size, peers, main, width), bf16), vm((tp_size, peers, spare_h, width), bf16),
            vm((4, total, width), bf16), vm((2, total, width), bf16),
            vm((total, width), bf16), vm((total, width), bf16),
            vm((peers, main, width), bf16), vm((peers, main, width), bf16),
            vm((peers, spare, width), f32), vm((peers, spare, width), f32),
            vm((1, padded), f32), vm((1, padded), f32), vm((1, padded), f32),
            vm((1, padded), f32), vm((1, padded), f32), vm((peers, 1, padded), f32),
            vm((total, hid), bf16),
            dma((3,)),
        ]
        + [dma((2, peers))] * 2 + [dma((peers,))] * 2
        + [dma((2, peers))] * 2 + [dma((peers,))] * 2
        + [dma((2, 2, peers))] * 2 + [dma((2, peers))] * 2
        + [dma((2,))] * 2 + [dma((len(chunks),))] * 2
        + [dma] * 4
        + [dma((peers,))] * 6,
        compiler_params=pltpu.CompilerParams(collective_id=0, has_side_effects=True),
    )(tokens, cotangent, routes.T, route_weights.T, gate_weight, up_weight, down_weight)
    return token_grad, weight_grad.T, down_grad


def per_device(tokens, cotangent, routes, route_weights, gate_weight, up_weight, down_weight):
    args = (tokens, cotangent, routes, route_weights, gate_weight, up_weight, down_weight)
    cap = routes.shape[0] * routes.shape[1] // lax.axis_size("ep") + 1
    peers = lax.axis_size("ep")
    small = cap < 16 or cap % 16 == 0 or cap > 127 or peers & (peers - 1) != 0
    if small or lax.axis_size("tp") != 4 or routes.shape[1] != 2 or peers > 16:
        return native(*args)
    return fused(*args)


def solution(mesh):
    placed = (
        P("ep", "tp"),
        P("ep", "tp"),
        P("ep", None),
        P("ep", None),
        P("ep", None, "tp"),
        P("ep", None, "tp"),
        P("ep", "tp", None),
    )
    return jax.shard_map(
        per_device,
        mesh=mesh,
        in_specs=placed,
        out_specs=(P("ep", "tp"), P("ep", None), P("ep", "tp", None)),
        check_vma=False,
    )
```

```python
import functools

import jax
import jax.numpy as jnp
from jax import lax
from jax.experimental import pallas as pl
from jax.experimental.pallas import tpu as pltpu
from jax.sharding import PartitionSpec as P

clamp_limit = 7.0
alpha_gate = 1.702
send_order = (1, 2, 3, 4, 5, 6, 7)
relay_lag = 6


def ranks_within(route_block, experts):
    flat_routes = route_block.reshape(-1)
    onehot = (flat_routes[:, None] == jnp.arange(experts, dtype=jnp.int32)[None, :]).astype(
        jnp.int32
    )
    before = jnp.cumsum(onehot, axis=0) - onehot
    return jnp.sum(before * onehot, axis=1)


def expert_terms(exp_rows, exp_grads, scales, gate_mat, up_mat, down_mat):
    gate_pre = jnp.dot(exp_rows, gate_mat, preferred_element_type=jnp.float32)
    up_pre = jnp.dot(exp_rows, up_mat, preferred_element_type=jnp.float32)
    gate_clip = jnp.minimum(gate_pre, clamp_limit)
    up_clip = jnp.clip(up_pre, -clamp_limit, clamp_limit)
    sigmoid_gate = jax.nn.sigmoid(alpha_gate * gate_clip)
    swish_gate = gate_clip * sigmoid_gate
    hidden = (up_clip + 1.0) * swish_gate
    back_proj = lax.dot_general(
        exp_grads, down_mat, (((1,), (1,)), ((), ())), preferred_element_type=jnp.float32
    )
    scores = jnp.sum(hidden * back_proj, axis=1)
    weight_col = scales.astype(jnp.float32)[:, None]
    scaled = back_proj * weight_col
    slope = sigmoid_gate + alpha_gate * swish_gate * (1.0 - sigmoid_gate)
    gate_grad = jnp.where(gate_pre < clamp_limit, scaled * (up_clip + 1.0) * slope, 0.0).astype(
        jnp.bfloat16
    )
    up_grad = jnp.where(jnp.abs(up_pre) < clamp_limit, scaled * swish_gate, 0.0).astype(
        jnp.bfloat16
    )
    weighted = (hidden * weight_col).astype(jnp.bfloat16)
    down_part = lax.dot_general(
        weighted, exp_grads, (((0,), (0,)), ((), ())), preferred_element_type=jnp.float32
    )
    token_part = lax.dot_general(
        gate_grad, gate_mat, (((1,), (1,)), ((), ())), preferred_element_type=jnp.float32
    )
    token_part = token_part + lax.dot_general(
        up_grad, up_mat, (((1,), (1,)), ((), ())), preferred_element_type=jnp.float32
    )
    return (token_part, scores, down_part)


def native(tokens, cotangent, routes, route_weights, gate_weight, up_weight, down_weight):
    experts = lax.axis_size("ep")
    tok_rows, top_count = routes.shape
    slots_each = tok_rows * top_count // experts + 1
    slot_count = experts * slots_each
    slot_ranks = ranks_within(routes, experts)
    slot_place = routes.reshape(-1) * slots_each + slot_ranks
    slot_owner = jnp.full((slot_count,), -1, jnp.int32)
    slot_owner = slot_owner.at[slot_place].set(jnp.arange(tok_rows * top_count, dtype=jnp.int32))
    filled = slot_owner >= 0
    pair_index = jnp.where(filled, slot_owner, 0)
    token_index = pair_index // top_count
    send_scales = jnp.where(filled, route_weights.reshape(-1)[pair_index], 0)
    send_rows = jnp.where(filled[:, None], tokens[token_index], 0)
    send_grads = jnp.where(filled[:, None], cotangent[token_index], 0)
    part_rows, part_grads, scales = (
        lax.all_to_all(send_rows, "ep", split_axis=0, concat_axis=0, tiled=True),
        lax.all_to_all(send_grads, "ep", split_axis=0, concat_axis=0, tiled=True),
        lax.all_to_all(send_scales, "ep", split_axis=0, concat_axis=0, tiled=True),
    )
    exp_rows, exp_grads = (
        lax.all_gather(part_rows, "tp", axis=1, tiled=True),
        lax.all_gather(part_grads, "tp", axis=1, tiled=True),
    )
    token_part, scores, down_part = expert_terms(
        exp_rows, exp_grads, scales, gate_weight[0], up_weight[0], down_weight[0]
    )
    token_share = lax.psum_scatter(
        token_part.astype(jnp.bfloat16), "tp", scatter_dimension=1, tiled=True
    )
    score_total = lax.psum(scores, "tp")
    back_rows, back_scores = (
        lax.all_to_all(token_share, "ep", split_axis=0, concat_axis=0, tiled=True),
        lax.all_to_all(
            score_total.astype(jnp.bfloat16), "ep", split_axis=0, concat_axis=0, tiled=True
        ),
    )
    pair_rows = back_rows[slot_place].reshape(tok_rows, top_count, back_rows.shape[1])
    token_grad = jnp.sum(pair_rows.astype(jnp.float32), axis=1).astype(jnp.bfloat16)
    weight_grad = back_scores[slot_place].reshape(tok_rows, top_count)
    return (token_grad, weight_grad, down_part.astype(jnp.bfloat16)[None])


def xor_index(value, mask):
    bit = 1
    while bit <= mask:
        if mask & bit:
            value = value + bit - 2 * bit * ((value // bit) % 2)
        bit *= 2
    return value


def dot_nn(a, b):
    return lax.dot_general(a, b, (((1,), (0,)), ((), ())), preferred_element_type=jnp.float32)


def dot_nt(a, b):
    return lax.dot_general(a, b, (((1,), (1,)), ((), ())), preferred_element_type=jnp.float32)


def dot_tn(a, b):
    return lax.dot_general(a, b, (((0,), (0,)), ((), ())), preferred_element_type=jnp.float32)


def fused_kernel(
    peers, main, spare, spare_rows, order, chunks,
    tokens_ref, cotangent_ref, routes_ref, scale_ref, gate_hbm, up_hbm, down_hbm,
    token_out, weight_out, down_out,
    gate_v, up_v, down_v, send_main, send_spare, rows_all, spare_all,
    part, core_part, y_send, y_part, ret_send, ret_recv, ret_spare_send, ret_spare_recv,
    score_own, score_core, score_sum, score_y, score_send, score_recv, weighted_v,
    w_sem, disp_s, disp_r, disp_es, disp_er, y_s, y_r, y_es, y_er,
    core_s, core_r, core_es, core_er,
    rs_s, rs_r, ry_s, ry_r, sc_s, sc_r, sy_s, sy_r,
    ret_s, ret_r, ret_es, ret_er, ret_ss, ret_sr,
):
    f32, bf16 = jnp.float32, jnp.bfloat16
    ep = lax.axis_index("ep")
    tp = lax.axis_index("tp")
    yy, cc = tp // 2, tp % 2
    other_y, other_c = 1 - yy, 1 - cc
    core_tp, y_tp, far_tp = yy * 2 + other_c, other_y * 2 + cc, other_y * 2 + other_c
    core_dev, y_dev = {"tp": core_tp}, {"tp": y_tp}

    def ep_dev(m):
        return {"ep": xor_index(ep, m)}

    barrier = pltpu.get_barrier_semaphore()
    devices = [ep_dev(m) for m in range(1, peers)] + [core_dev, y_dev]
    for device in devices:
        pl.semaphore_signal(
            barrier, inc=1, device_id=device, device_id_type=pl.DeviceIdType.MESH
        )
    loads = [
        pltpu.make_async_copy(gate_hbm.at[0], gate_v, w_sem.at[0]),
        pltpu.make_async_copy(up_hbm.at[0], up_v, w_sem.at[1]),
        pltpu.make_async_copy(down_hbm.at[0], down_v, w_sem.at[2]),
    ]
    for load in loads:
        load.start()

    tok, width = tokens_ref.shape
    base = peers * main
    slots = base + spare_rows
    padded = score_own.shape[1]
    group = 16

    def iota(shape, dim):
        return lax.broadcasted_iota(jnp.int32, shape, dim)

    m_col = iota((group, 1), 0)
    e_col = jnp.zeros((group, 1), jnp.int32)
    bit = 1
    while bit < peers:
        mine = (ep // bit) % 2
        have = jnp.where((m_col & bit) != 0, 1, 0)
        e_col = e_col + bit * (have + mine - 2 * have * mine)
        bit *= 2
    e_col = jnp.where(m_col < peers, e_col, -1)
    first = (routes_ref[0:1, :] == e_col).astype(f32)
    second = (routes_ref[1:2, :] == e_col).astype(f32)
    named = first + second
    tri = (iota((tok, tok), 0) <= iota((tok, tok), 1)).astype(f32).astype(bf16)
    rank1 = named * dot_nn(named.astype(bf16), tri)
    scale = scale_ref[...].astype(f32)
    scale_m = (first * scale[0:1, :] + second * scale[1:2, :]).astype(bf16)

    def in_block(place, m):
        in_main = (place >= m * main) & (place < m * main + main)
        low = base + m * spare
        return in_main | ((place >= low) & (place < low + spare))

    expand = in_block(iota((slots, group), 0), iota((slots, group), 1))
    expand = (expand & (iota((slots, group), 1) < peers)).astype(f32).astype(bf16)
    s_col = iota((slots, 1), 0)
    t_main = s_col + 1
    t_spare = s_col - base + 1 + main
    for m in range(1, peers):
        t_main = t_main - jnp.where(s_col >= m * main, main, 0)
        t_spare = t_spare - jnp.where(s_col - base >= m * spare, spare, 0)
    target = jnp.where(s_col < base, t_main, jnp.where(s_col < base + peers * spare, t_spare, -5))
    ranks_s = dot_nn(expand, rank1.astype(bf16))
    pick = (ranks_s == target.astype(f32)).astype(f32).astype(bf16)
    pick_pad = jnp.concatenate([pick, jnp.zeros((padded - slots, tok), bf16)], axis=0)

    x_slots = dot_nn(pick, tokens_ref[...])
    x_main = x_slots[:base].astype(bf16).reshape(peers, main, width)
    send_main[0] = x_main
    rows_all[0, tp, 0] = x_main[0]
    g_slots = dot_nn(pick, cotangent_ref[...])
    g_main = g_slots[:base].astype(bf16).reshape(peers, main, width)
    send_main[1] = g_main
    rows_all[1, tp, 0] = g_main[0]
    w_rows = dot_nt(scale_m, pick_pad)
    w_rows = jnp.concatenate([w_rows, jnp.zeros((group, width - padded), f32)], axis=1)
    spare_h = 2 * spare + 1
    row_id = iota((spare_h, width), 0)
    for m in range(peers):
        block = jnp.broadcast_to(w_rows[m : m + 1], (spare_h, width))
        for x in range(spare):
            j = base + m * spare + x
            block = jnp.where(row_id == x, x_slots[j : j + 1], block)
            block = jnp.where(row_id == spare + x, g_slots[j : j + 1], block)
        block = block.astype(bf16)
        send_spare[m] = block
        if m == 0:
            spare_all[tp, 0] = block

    pl.semaphore_wait(barrier, len(devices))

    pending = []

    def remote(src, dst, s_sem, r_sem, device):
        copy = pltpu.make_async_remote_copy(
            src_ref=src, dst_ref=dst, send_sem=s_sem, recv_sem=r_sem,
            device_id=device, device_id_type=pl.DeviceIdType.MESH,
        )
        copy.start()
        pending.append(copy)
        return copy

    disp, y_copy, core_a, core_b = {}, {}, {}, {}

    def dispatch(w, m):
        disp[w, m] = [
            remote(send_main.at[w, m], rows_all.at[w, tp, m], disp_s.at[w, m], disp_r.at[w, m], ep_dev(m))
        ]
        if w == 0:
            disp[w, m].append(
                remote(send_spare.at[m], spare_all.at[tp, m], disp_es.at[m], disp_er.at[m], ep_dev(m))
            )

    def forward(w, m):
        if m > 0:
            for copy in disp[w, m]:
                copy.wait_recv()
        src = rows_all.at[w, tp, m] if m > 0 else send_main.at[w, 0]
        dst = rows_all.at[w, tp, m]
        y_copy[w, m] = [remote(src, dst, y_s.at[w, m], y_r.at[w, m], y_dev)]
        core_a[w, m] = [remote(src, dst, core_s.at[0, w, m], core_r.at[0, w, m], core_dev)]
        if w == 0:
            src = spare_all.at[tp, m] if m > 0 else send_spare.at[0]
            dst = spare_all.at[tp, m]
            y_copy[w, m].append(remote(src, dst, y_es.at[m], y_er.at[m], y_dev))
            core_a[w, m].append(remote(src, dst, core_es.at[0, m], core_er.at[0, m], core_dev))

    def relay(w, m):
        for copy in y_copy[w, m]:
            copy.wait_recv()
        block = rows_all.at[w, y_tp, m]
        core_b[w, m] = [remote(block, block, core_s.at[1, w, m], core_r.at[1, w, m], core_dev)]
        if w == 0:
            block = spare_all.at[y_tp, m]
            core_b[w, m].append(remote(block, block, core_es.at[1, m], core_er.at[1, m], core_dev))

    def settle(copies, w):
        for m in range(peers):
            for copy in copies[w, m]:
                copy.wait_recv()

    tp_size = rows_all.shape[1]
    wide_row = iota((spare_rows, width), 0)

    def spare_tile(which, t):
        tile = jnp.zeros((spare_rows, width), f32)
        for m in range(peers):
            block = spare_all[t, m].astype(f32)
            for x in range(spare):
                row = which * spare + x
                tile = jnp.where(wide_row == m * spare + x, block[row : row + 1], tile)
        return tile.astype(bf16)

    def rows_of(which, t):
        block = rows_all[which, t].reshape(base, width)
        return jnp.concatenate([block, spare_tile(which, t)], axis=0)

    def cut(t):
        return pl.ds(pl.multiple_of(t * width, width), width)

    for m in order:
        dispatch(0, m)
    for m in order:
        dispatch(1, m)
    turn = (0,) + order
    items = [(w, m) for w in range(2) for m in turn]
    sums = {}

    def add(name, term):
        sums[name] = sums[name] + term if name in sums else term

    def front(t):
        x_t = rows_of(0, t)
        add("gate", dot_nn(x_t, gate_v[cut(t), :]))
        add("up", dot_nn(x_t, up_v[cut(t), :]))

    def gates():
        gate_pre, up_pre = sums["gate"], sums["up"]
        s_lane = iota((1, padded), 1)
        w_row = jnp.zeros((1, padded), f32)
        for m in range(peers):
            row = spare_all[0, m].astype(f32)[2 * spare : 2 * spare + 1, 0:padded]
            w_row = jnp.where(in_block(s_lane, m), row, w_row)
        eye_b = (iota((slots, padded), 0) == iota((slots, padded), 1)).astype(f32).astype(bf16)
        weight_col = dot_nt(eye_b, jnp.broadcast_to(w_row, (group, padded)).astype(bf16))[:, 0:1]
        gate_clip = jnp.minimum(gate_pre, clamp_limit)
        up_clip = jnp.clip(up_pre, -clamp_limit, clamp_limit)
        sigmoid_gate = jax.nn.sigmoid(alpha_gate * gate_clip)
        swish_gate = gate_clip * sigmoid_gate
        hidden = (up_clip + 1.0) * swish_gate
        slope = sigmoid_gate + alpha_gate * swish_gate * (1.0 - sigmoid_gate)
        weighted_v[...] = (hidden * weight_col).astype(bf16)
        gate_fac = jnp.where(gate_pre < clamp_limit, weight_col * (up_clip + 1.0) * slope, 0.0)
        up_fac = jnp.where(jnp.abs(up_pre) < clamp_limit, weight_col * swish_gate, 0.0)
        return hidden, gate_fac, up_fac

    hooks = [
        (peers, lambda: front(tp)),
        (peers + 1, lambda: (settle(core_a, 0), front(core_tp))),
        (peers + relay_lag, lambda: front(y_tp)),
        (peers + relay_lag + 1, lambda: (settle(core_b, 0), front(far_tp))),
        (peers + relay_lag + 2, lambda: factors.append(gates())),
    ]
    factors = []
    for i in range(2 * peers + relay_lag):
        if i < 2 * peers:
            forward(*items[i])
        if i >= relay_lag:
            relay(*items[i - relay_lag])
        if i == peers:
            for load in loads:
                load.wait()
        for when, hook in hooks:
            if when == i:
                hook()
    hidden, gate_fac, up_fac = factors[0]
    back = dot_nt(rows_of(1, tp), down_v[:, cut(tp)])
    settle(core_a, 1)
    back = back + dot_nt(rows_of(1, core_tp), down_v[:, cut(core_tp)])
    back = back + dot_nt(rows_of(1, y_tp), down_v[:, cut(y_tp)])
    settle(core_b, 1)
    back = back + dot_nt(rows_of(1, far_tp), down_v[:, cut(far_tp)])
    gate_grad = (back * gate_fac).astype(bf16)
    up_grad = (back * up_fac).astype(bf16)

    def piece(t):
        return dot_nt(gate_grad, gate_v[cut(t), :]) + dot_nt(up_grad, up_v[cut(t), :])

    part[2] = piece(far_tp).astype(bf16)
    rs_far = remote(part.at[2], core_part.at[0], rs_s.at[0], rs_r.at[0], core_dev)
    scores = jnp.sum(hidden * back, axis=1, keepdims=True)
    eye = iota((slots, padded), 0) == iota((slots, padded), 1)
    score_own[...] = jnp.sum(jnp.where(eye, scores, 0.0), axis=0, keepdims=True)
    small = remote(score_own, score_core, sc_s, sc_r, core_dev)
    part[3] = piece(core_tp).astype(bf16)
    rs_near = remote(part.at[3], core_part.at[1], rs_s.at[1], rs_r.at[1], core_dev)
    mine = piece(y_tp).astype(bf16).astype(f32)
    small.wait_recv()
    score_sum[...] = score_own[...] + score_core[...]
    small_y = remote(score_sum, score_y, sy_s, sy_r, y_dev)
    rs_far.wait_recv()
    y_send[...] = (mine + core_part[0].astype(f32)).astype(bf16)
    ry = []
    for q, (lo, hi) in enumerate(chunks):
        rows = pl.ds(lo * main, (hi - lo) * main + (spare_rows if hi == peers else 0))
        ry.append(remote(y_send.at[rows], y_part.at[rows], ry_s.at[q], ry_r.at[q], y_dev))
    mine = piece(tp).astype(bf16).astype(f32)
    rs_near.wait_recv()
    part[0] = mine.astype(bf16)
    returns = []
    for q, (lo, hi) in enumerate(chunks):
        row_lo, row_n = lo * main, (hi - lo) * main
        row_n = row_n + (spare_rows if hi == peers else 0)
        ry[q].wait_recv()
        total = (
            part[0, row_lo : row_lo + row_n, :].astype(f32)
            + core_part[1, row_lo : row_lo + row_n, :].astype(f32)
            + y_part[row_lo : row_lo + row_n, :].astype(f32)
        )
        ret_send[lo:hi] = total[: (hi - lo) * main].astype(bf16).reshape(hi - lo, main, width)
        for m in reversed(range(max(lo, 1), hi)):
            returns.append(remote(ret_send.at[m], ret_recv.at[m], ret_s.at[m], ret_r.at[m], ep_dev(m)))
        if q == 0:
            small_y.wait_recv()
            score_send[...] = score_sum[...] + score_y[...]
            for m in range(1, peers):
                returns.append(remote(score_send, score_recv.at[m], ret_ss.at[m], ret_sr.at[m], ep_dev(m)))
        if hi == peers:
            for m in range(peers):
                for x in range(spare):
                    j = (hi - lo) * main + m * spare + x
                    ret_spare_send[m, x : x + 1] = total[j : j + 1]
            for m in range(1, peers):
                returns.append(
                    remote(ret_spare_send.at[m], ret_spare_recv.at[m], ret_es.at[m], ret_er.at[m], ep_dev(m))
                )
    weighted = weighted_v[...]
    for t in range(tp_size):
        down_out[0, :, t * width : (t + 1) * width] = dot_tn(weighted, rows_of(1, t)).astype(bf16)
    for copy in returns:
        copy.wait_recv()
    back_rows = [ret_send[0]] + [ret_recv[m] for m in range(1, peers)]
    tile = jnp.zeros((spare_rows, width), f32)
    s_lane = iota((1, padded), 1)
    group_row = iota((group, padded), 0)
    score_mat = jnp.zeros((group, padded), f32)
    for m in range(peers):
        block = ret_spare_send[0] if m == 0 else ret_spare_recv[m]
        for x in range(spare):
            tile = jnp.where(wide_row == m * spare + x, block[x : x + 1], tile)
        row = score_send[...] if m == 0 else score_recv[m]
        score_mat = jnp.where(group_row == m, jnp.where(in_block(s_lane, m), row, 0.0), score_mat)
    back_all = jnp.concatenate(back_rows + [tile.astype(bf16)], axis=0)
    token_out[...] = dot_tn(pick, back_all).astype(bf16)
    found = dot_nn(score_mat.astype(bf16), pick_pad)
    row0 = jnp.sum(first * found, axis=0, keepdims=True)
    row1 = jnp.sum(second * found, axis=0, keepdims=True)
    weight_out[...] = jnp.where(iota((2, tok), 0) == 0, row0, row1).astype(bf16)
    for copy in pending:
        copy.wait_send()


def fused(tokens, cotangent, routes, route_weights, gate_weight, up_weight, down_weight):
    peers = lax.axis_size("ep")
    tp_size = lax.axis_size("tp")
    tok, top_count = routes.shape
    width = tokens.shape[1]
    cap = tok * top_count // peers + 1
    main = cap // 16 * 16
    spare = cap - main
    spare_rows = -(-(peers * spare) // 16) * 16
    total = peers * main + spare_rows
    padded = -(-total // 128) * 128
    hid, full = down_weight.shape[1], down_weight.shape[2]
    order = send_order if len(send_order) == peers - 1 else tuple(range(1, peers))
    pieces = min(8, peers)
    chunks = [(q * peers // pieces, (q + 1) * peers // pieces) for q in reversed(range(pieces))]
    bf16, f32 = jnp.bfloat16, jnp.float32
    vm = pltpu.VMEM
    dma = pltpu.SemaphoreType.DMA
    any_spec = pl.BlockSpec(memory_space=pl.ANY)
    v_spec = pl.BlockSpec(memory_space=pltpu.VMEM)
    spare_h = 2 * spare + 1
    token_grad, weight_grad, down_grad = pl.pallas_call(
        functools.partial(fused_kernel, peers, main, spare, spare_rows, order, chunks),
        out_shape=(
            pltpu.VMEM((tok, width), bf16),
            pltpu.VMEM((top_count, tok), bf16),
            pltpu.VMEM((1, hid, full), bf16),
        ),
        in_specs=[v_spec] * 4 + [any_spec] * 3,
        out_specs=(v_spec, v_spec, v_spec),
        scratch_shapes=[
            vm((full, hid), bf16), vm((full, hid), bf16), vm((hid, full), bf16),
            vm((2, peers, main, width), bf16), vm((peers, spare_h, width), bf16),
            vm((2, tp_size, peers, main, width), bf16), vm((tp_size, peers, spare_h, width), bf16),
            vm((4, total, width), bf16), vm((2, total, width), bf16),
            vm((total, width), bf16), vm((total, width), bf16),
            vm((peers, main, width), bf16), vm((peers, main, width), bf16),
            vm((peers, spare, width), f32), vm((peers, spare, width), f32),
            vm((1, padded), f32), vm((1, padded), f32), vm((1, padded), f32),
            vm((1, padded), f32), vm((1, padded), f32), vm((peers, 1, padded), f32),
            vm((total, hid), bf16),
            dma((3,)),
        ]
        + [dma((2, peers))] * 2 + [dma((peers,))] * 2
        + [dma((2, peers))] * 2 + [dma((peers,))] * 2
        + [dma((2, 2, peers))] * 2 + [dma((2, peers))] * 2
        + [dma((2,))] * 2 + [dma((len(chunks),))] * 2
        + [dma] * 4
        + [dma((peers,))] * 6,
        compiler_params=pltpu.CompilerParams(collective_id=0, has_side_effects=True),
    )(tokens, cotangent, routes.T, route_weights.T, gate_weight, up_weight, down_weight)
    return token_grad, weight_grad.T, down_grad


def per_device(tokens, cotangent, routes, route_weights, gate_weight, up_weight, down_weight):
    args = (tokens, cotangent, routes, route_weights, gate_weight, up_weight, down_weight)
    cap = routes.shape[0] * routes.shape[1] // lax.axis_size("ep") + 1
    peers = lax.axis_size("ep")
    small = cap < 16 or cap % 16 == 0 or cap > 127 or peers & (peers - 1) != 0
    if small or lax.axis_size("tp") != 4 or routes.shape[1] != 2 or peers > 16:
        return native(*args)
    return fused(*args)


def solution(mesh):
    placed = (
        P("ep", "tp"),
        P("ep", "tp"),
        P("ep", None),
        P("ep", None),
        P("ep", None, "tp"),
        P("ep", None, "tp"),
        P("ep", "tp", None),
    )
    return jax.shard_map(
        per_device,
        mesh=mesh,
        in_specs=placed,
        out_specs=(P("ep", "tp"), P("ep", None), P("ep", "tp", None)),
        check_vma=False,
    )
```
